512 devices in a mesh: fs: 64 (over z, y), tp: 8 (over x, core).
Axes of the slice: x: 4, y: 8, z: 8, core: 2. Of those that a mesh axis runs over, the one named last changes fastest.
Arguments:
- inputs: bfloat16 [32768, 2048], P('fs', 'tp'), may hold values from -6 to 6
- hidden_pre: bfloat16 [32768, 4096], P('fs', 'tp'), may hold values from -6 to 6
- norm_input: bfloat16 [32768, 2048], P('fs', 'tp'), may hold values from -48 to 48, as said below
- out_gain: float32 [2048], P('tp'), may hold values from 0.1 to 1.9
- w_up: bfloat16 [2048, 4096], P('tp', 'fs'), may hold values from -0.125 to 0.125
- w_down: bfloat16 [4096, 2048], P('tp', 'fs'), may hold values from -0.09375 to 0.09375
- cotangent: bfloat16 [32768, 2048], P('fs', 'tp'), may hold values from -16 to 16
Outputs:
- grad_input: bfloat16 [32768, 2048], P('fs', 'tp')
- grad_up: float32 [2048, 4096], P('tp', 'fs')
- grad_gain: float32 [2048], P('tp')
The draws below stay inside these ranges and needn't reach their ends.
Inputs may be any that keep to these rules, and one draw needn't show every extreme that they name: `norm_input`: each token's features are scaled by a factor of that token, and each block of 2048 / 8 features by a factor of that block.
All inputs are finite; a program needn't handle non-finite values.
Results may differ from the reference program's by a relative error of at most 0.0058.
Values may be sent and summed in bfloat16 or wider, within the bound.
No kernel may reach another device: no remote copies, remote signals or barrier semaphores. Data moves between devices by JAX's collectives and lax.ppermute only.
A program may use at most 64 MiB of HBM per device.

```python
import jax
import jax.numpy as jnp
from jax import lax

D = 2048
FF = 4096
TOKENS = 32768
N_TP = 8


def draw_norm_input(key, part):
    key_base, key_block, key_row, key_common = jax.random.split(key, 4)
    base = jnp.clip(jax.random.normal(key_base, (TOKENS, D), jnp.float32), -6.0, 6.0)
    blocks = jnp.exp(jax.random.uniform(key_block, (N_TP,), jnp.float32, -1.2, 1.2))
    columns = jnp.repeat(blocks, D // N_TP)
    rowwise = jnp.exp(jax.random.uniform(key_row, (TOKENS, 1), jnp.float32, -0.7, 0.7))
    return (base * rowwise * columns[None, :]).astype(jnp.bfloat16)


def raised(entries, key, source, target, shards_of, factor):
    def block_of(dim):
        return (jnp.arange(entries.shape[dim]) // (entries.shape[dim] // shards_of)).reshape((-1,) + (1,) * (entries.ndim - 1 - dim))

    one_side = jax.random.permutation(key, shards_of)[block_of(target)]
    other_side = (block_of(target) + shards_of // 2) % shards_of
    return jnp.where((block_of(source) == one_side) | (block_of(source) == other_side), factor * entries, entries)


def block_scale(rng, dims, pieces, least, largest):
    factor_of = 1.0
    for position, blocks in pieces:
        draws = jax.random.uniform(jax.random.fold_in(jax.random.fold_in(rng, 6), position), (blocks,), jnp.float32, least / len(pieces), largest / len(pieces))
        factor_of = factor_of * jnp.repeat(jnp.exp(draws), dims[position] // blocks).reshape((-1,) + (1,) * (len(dims) - 1 - position))
    return factor_of


def normal_values(key, dims, deviation, limit, pieces=(), dtype=jnp.bfloat16):
    level = block_scale(key, dims, pieces, -0.22, 0.18) if pieces else 1.0
    entries = jax.random.normal(key, dims, jnp.float32) * deviation * level
    return jnp.minimum(jnp.maximum(entries, -limit), limit).astype(dtype)


def noise_with(own_key, dims, width, bound, cuts, heavy, held_as=jnp.bfloat16):
    result = width * jax.random.normal(own_key, dims, jnp.float32)
    if cuts:
        result = result * block_scale(own_key, dims, cuts, -0.22, 0.18)
    return jnp.clip(raised(result, jax.random.fold_in(own_key, 3), *heavy), -bound, bound).astype(held_as)


def setup_inputs(seed: int = 0) -> dict:
    arg_keys = jax.random.split(jax.random.key(seed), 8)
    inputs = normal_values(arg_keys[0], (TOKENS, D), 1.0, 6.0, ((0, 64), (1, 8)))
    hidden_pre = normal_values(arg_keys[1], (TOKENS, FF), 1.0, 6.0, ((0, 64), (1, 8)))
    norm_input = draw_norm_input(jax.random.fold_in(arg_keys[7], 71), 0)
    out_gain = jnp.clip(1.0 + 0.18 * jax.random.normal(arg_keys[3], (D,), jnp.float32), 0.1, 1.9)
    w_up = normal_values(arg_keys[4], (D, FF), D ** -0.5, 0.125, ((0, 8), (1, 64)))
    w_down = normal_values(arg_keys[5], (FF, D), FF ** -0.5, 0.09375, ((0, 8), (1, 64)))
    cotangent = noise_with(arg_keys[6], (TOKENS, D), 1.0, 16.0, ((0, 64), (1, 8)), (0, 1, 64, 4.0))
    return dict(inputs=inputs, hidden_pre=hidden_pre, norm_input=norm_input, out_gain=out_gain, w_up=w_up, w_down=w_down, cotangent=cotangent)


norm_eps = 1e-06

def reference(inputs, hidden_pre, norm_input, out_gain, w_up, w_down, cotangent):
    scaled = TOKENS ** (-0.5)
    normed = norm_input.astype(jnp.float32)
    upstream = cotangent.astype(jnp.float32)
    inv_rms = lax.rsqrt(lax.optimization_barrier(jnp.mean(normed * normed, axis=1, keepdims=True)) + norm_eps)
    cross_mean = lax.optimization_barrier(jnp.mean(upstream * out_gain * normed, axis=1, keepdims=True))
    d_out = (upstream * out_gain * inv_rms - normed * inv_rms * inv_rms * inv_rms * cross_mean).astype(jnp.bfloat16)
    grad_gain = lax.optimization_barrier(jnp.sum(upstream * normed * inv_rms, axis=0)) * scaled
    d_act = jnp.dot(d_out, w_down.T, preferred_element_type=jnp.float32)
    d_pre = (d_act * 2.0 * jax.nn.relu(hidden_pre.astype(jnp.float32))).astype(jnp.bfloat16)
    grad_input = jnp.dot(d_pre, w_up.T, preferred_element_type=jnp.float32).astype(jnp.bfloat16)
    grad_up = jnp.dot(inputs.T, d_pre, preferred_element_type=jnp.float32) * scaled
    return (grad_input, grad_up, grad_gain)
```

```python
import jax
import jax.numpy as jnp
from jax import lax
from jax.experimental import pallas as pl
from jax.sharding import Mesh
from jax.sharding import PartitionSpec as P

FS = ("z", "y")
bf16 = jnp.bfloat16
f32 = jnp.float32
norm_eps = 1e-06


def exchange(chunks, axis):
    return lax.all_to_all(chunks, axis, 0, 0, tiled=True)


def gather_directly(value, axis):
    n = lax.axis_size(axis)
    return exchange(jnp.broadcast_to(value[None], (n, *value.shape)), axis)


def summed(parts):
    return jnp.sum(parts.astype(f32), axis=0)


def after(value, earlier):
    return lax.optimization_barrier((value, earlier))[0]


def grad_up_kernel(dout, wd, hidden, inputs, d_pre_out, g_out):
    blocks, toks, feats = dout.shape
    half = wd.shape[-1]
    for s in range(2):
        cols = slice(s * half, (s + 1) * half)
        acc = jnp.zeros((toks, half), f32)
        for k in range(blocks):
            w = wd[k, :, s].reshape(feats, half)
            acc += jnp.dot(dout[k], w, preferred_element_type=f32)
        pre = jnp.maximum(hidden[:, cols].astype(f32), 0.0)
        d_pre_out[:, cols] = (acc * 2.0 * pre).astype(bf16)
    d_pre_t = d_pre_out[...].T
    for k in range(blocks):
        g_out[k] = jnp.dot(d_pre_t, inputs[k], preferred_element_type=f32).astype(bf16)


def grad_input_kernel(d_pre, w_up, out):
    left = d_pre[...]
    for k in range(out.shape[0]):
        out[k] = jnp.dot(left, w_up[k], preferred_element_type=f32).astype(bf16)


def one_device(inputs, hidden_pre, norm_input, out_gain, w_up, w_down, cotangent):
    nz, ny, ntp = (lax.axis_size(a) for a in ("z", "y", "tp"))
    toks, feats = inputs.shape
    hid = hidden_pre.shape[1]
    width = feats * ntp
    scaled = (toks * nz * ny) ** (-0.5)
    swap = [(a * ntp + b, b * ntp + a) for a in range(nz) for b in range(ntp)]

    normed = norm_input.astype(f32)
    upstream = cotangent.astype(f32)
    weighted = upstream * out_gain
    sums = jnp.stack([jnp.sum(normed * normed, axis=1), jnp.sum(weighted * normed, axis=1)])

    wd = w_down.T
    half = hid // 2
    both = jnp.concatenate([wd[:, :half], wd[:, half:], w_up.T], axis=0)
    both = gather_directly(both, "y")
    wd_rows = 2 * wd.shape[0]
    wd = wd_y = both[:, :wd_rows].reshape(ny * wd_rows, half)
    wd = lax.all_gather(wd, "z", axis=0, tiled=True)
    wd = wd.reshape(nz, ny, 2, wd_rows // 2, half)
    wu = both[:, wd_rows:].reshape(hid, feats)
    wu = lax.ppermute(wu, ("z", "tp"), swap)

    sums = gather_directly(after(sums, wd_y), "tp")
    sums = jnp.sum(sums, axis=0)
    inv_rms = lax.rsqrt(sums[0] / width + norm_eps)[:, None]
    cross_mean = (sums[1] / width)[:, None]
    d_out = (weighted * inv_rms - normed * inv_rms * inv_rms * inv_rms * cross_mean).astype(bf16)
    gain_part = jnp.sum(upstream * normed * inv_rms, axis=0) * scaled
    dout_all = lax.all_gather(d_out, "tp", axis=0, tiled=True)
    dout_all = dout_all.reshape(ntp, toks, feats)
    inputs_all = gather_directly(after(inputs, sums), "tp")
    wu = lax.all_gather(after(wu, inputs_all), "z", axis=0, tiled=True).reshape(nz, hid, feats)

    d_pre, g = pl.pallas_call(
        grad_up_kernel,
        out_shape=(
            jax.ShapeDtypeStruct((toks, hid), bf16),
            jax.ShapeDtypeStruct((nz, hid, feats), bf16),
        ),
        name="grad_up_part",
    )(dout_all, wd, hidden_pre, inputs_all)

    grad_gain = jnp.sum(gather_directly(after(gain_part, d_pre), FS), axis=0)

    g = lax.psum_scatter(g.reshape(nz * hid, feats), "z", scatter_dimension=0, tiled=True)
    g = after(g, grad_gain)
    g = summed(exchange(g.reshape(ny, hid // ny, feats), "y")) * scaled
    grad_up = lax.ppermute(g, ("z", "tp"), swap).T

    part = pl.pallas_call(
        grad_input_kernel,
        out_shape=jax.ShapeDtypeStruct((ntp, toks, feats), bf16),
        name="grad_input_part",
    )(d_pre, wu)
    part = part.reshape(ntp * toks, feats)
    grad_input = lax.psum_scatter(part, "tp", scatter_dimension=0, tiled=True)

    return (grad_input, grad_up, grad_gain)


def solution(mesh):
    torus = Mesh(mesh.devices.reshape(8, 8, mesh.shape["tp"]), ("z", "y", "tp"))
    in_specs = (
        P(FS, "tp"),
        P(FS, "tp"),
        P(FS, "tp"),
        P("tp"),
        P("tp", FS),
        P("tp", FS),
        P(FS, "tp"),
    )
    out_specs = (P(FS, "tp"), P("tp", FS), P("tp"))
    return jax.shard_map(
        one_device, mesh=torus, in_specs=in_specs, out_specs=out_specs, check_vma=False
    )
```

```python
import jax
import jax.numpy as jnp
from jax import lax
from jax.experimental import pallas as pl
from jax.sharding import Mesh
from jax.sharding import PartitionSpec as P

FS = ("z", "y")
bf16 = jnp.bfloat16
f32 = jnp.float32
norm_eps = 1e-06


def exchange(chunks, axis):
    return lax.all_to_all(chunks, axis, 0, 0, tiled=True)


def gather_directly(value, axis):
    n = lax.axis_size(axis)
    return exchange(jnp.broadcast_to(value[None], (n, *value.shape)), axis)


def summed(parts):
    return jnp.sum(parts.astype(f32), axis=0)


def after(value, earlier):
    return lax.optimization_barrier((value, earlier))[0]


def butterfly(value, axes):
    for axis in axes:
        n = lax.axis_size(axis)
        step = 1
        while step < n:
            value = value + lax.ppermute(value, axis, [(i, i ^ step) for i in range(n)])
            step *= 2
    return value


def grad_up_kernel(dout, wd, hidden, inputs, d_pre_out, g_out):
    blocks, toks, feats = dout.shape
    half = wd.shape[-1]
    for s in range(2):
        cols = slice(s * half, (s + 1) * half)
        acc = jnp.zeros((toks, half), f32)
        for k in range(blocks):
            w = wd[k, :, s].reshape(feats, half)
            acc += jnp.dot(dout[k], w, preferred_element_type=f32)
        pre = jnp.maximum(hidden[:, cols].astype(f32), 0.0)
        d_pre_out[:, cols] = (acc * 2.0 * pre).astype(bf16)
    d_pre_t = d_pre_out[...].T
    rows = g_out.shape[1]
    for k in range(blocks):
        g = jnp.dot(d_pre_t, inputs[k], preferred_element_type=f32).astype(bf16)
        for j in range(blocks):
            g_out[k * blocks + j] = g[j * rows : (j + 1) * rows]


def grad_input_kernel(d_pre, w_up, out):
    left = d_pre[...]
    for k in range(out.shape[0]):
        out[k] = jnp.dot(left, w_up[k], preferred_element_type=f32).astype(bf16)


def one_device(inputs, hidden_pre, norm_input, out_gain, w_up, w_down, cotangent):
    nz, ny, ntp = (lax.axis_size(a) for a in ("z", "y", "tp"))
    toks, feats = inputs.shape
    hid = hidden_pre.shape[1]
    width = feats * ntp
    scaled = (toks * nz * ny) ** (-0.5)
    swap = [(a * ntp + b, b * ntp + a) for a in range(nz) for b in range(ntp)]

    normed = norm_input.astype(f32)
    upstream = cotangent.astype(f32)
    weighted = upstream * out_gain
    sums = jnp.stack([jnp.sum(normed * normed, axis=1), jnp.sum(weighted * normed, axis=1)])

    inputs_all = lax.all_gather(inputs, "tp", axis=0, tiled=True).reshape(ntp, toks, feats)
    wd = w_down.T
    half = hid // 2
    both = jnp.concatenate([wd[:, :half], wd[:, half:], w_up.T], axis=0)
    both = gather_directly(both, "y")
    wd_rows = 2 * wd.shape[0]
    wd = wd_y = both[:, :wd_rows].reshape(ny * wd_rows, half)
    wd = lax.all_gather(wd, "z", axis=0, tiled=True).reshape(nz, ny, 2, wd_rows // 2, half)
    wu = both[:, wd_rows:].reshape(hid, feats)
    wu = lax.ppermute(after(wu, wd_y), ("z", "tp"), swap)

    sums = jnp.sum(gather_directly(after(sums, wd_y), "tp"), axis=0)
    inv_rms = lax.rsqrt(sums[0] / width + norm_eps)[:, None]
    cross_mean = (sums[1] / width)[:, None]
    d_out = (weighted * inv_rms - normed * inv_rms * inv_rms * inv_rms * cross_mean).astype(bf16)
    gain_part = jnp.sum(upstream * normed * inv_rms, axis=0) * scaled
    dout_all = gather_directly(d_out, "tp")

    d_pre, g = pl.pallas_call(
        grad_up_kernel,
        out_shape=(
            jax.ShapeDtypeStruct((toks, hid), bf16),
            jax.ShapeDtypeStruct((nz * ny, hid // ny, feats), bf16),
        ),
        name="grad_up_part",
    )(dout_all, wd, hidden_pre, inputs_all)

    g = exchange(g, FS)
    g = summed(g) * scaled
    grad_up = lax.ppermute(g, ("z", "tp"), swap).T

    grad_gain = butterfly(after(gain_part, d_pre), ("z", "y"))

    wu = lax.all_gather(after(wu, dout_all), "z", axis=0, tiled=True).reshape(nz, hid, feats)
    part = pl.pallas_call(
        grad_input_kernel,
        out_shape=jax.ShapeDtypeStruct((ntp, toks, feats), bf16),
        name="grad_input_part",
    )(after(d_pre, grad_gain), wu)
    part = part.reshape(ntp * toks, feats)
    grad_input = lax.psum_scatter(part, "tp", scatter_dimension=0, tiled=True)

    return (grad_input, grad_up, grad_gain)


def solution(mesh):
    torus = Mesh(mesh.devices.reshape(8, 8, mesh.shape["tp"]), ("z", "y", "tp"))
    in_specs = (
        P(FS, "tp"),
        P(FS, "tp"),
        P(FS, "tp"),
        P("tp"),
        P("tp", FS),
        P("tp", FS),
        P(FS, "tp"),
    )
    out_specs = (P(FS, "tp"), P("tp", FS), P("tp"))
    return jax.shard_map(
        one_device, mesh=torus, in_specs=in_specs, out_specs=out_specs, check_vma=False
    )
```

```python
import jax
import jax.numpy as jnp
from jax import lax
from jax.experimental import pallas as pl
from jax.experimental.pallas import tpu as pltpu
from jax.sharding import Mesh
from jax.sharding import PartitionSpec as P

FS = ("z", "y")
TP = ("x", "c")
bf16 = jnp.bfloat16
f32 = jnp.float32
norm_eps = 1e-06


def exchange(chunks, axis):
    return lax.all_to_all(chunks, axis, 0, 0, tiled=True)


def gather_directly(value, axis):
    n = lax.axis_size(axis)
    return exchange(jnp.broadcast_to(value[None], (n, *value.shape)), axis)


def gather_two_steps(value):
    mine = gather_directly(value, "x")
    theirs = lax.ppermute(mine, "c", [(0, 1), (1, 0)])
    return mine, theirs


def after(value, earlier):
    return lax.optimization_barrier((value, earlier))[0]


def summed(parts):
    return jnp.sum(parts.astype(f32), axis=0)


def d_pre_kernel(core, mine, theirs, wd, hidden, out):
    chips, toks, feats = mine.shape
    half = wd.shape[-1]
    c = core[0]
    for s in range(2):
        cols = slice(s * half, (s + 1) * half)
        acc = jnp.zeros((toks, half), f32)
        for k in range(chips):
            w = wd[2 * k + c, :, s].reshape(feats, half)
            acc += jnp.dot(mine[k], w, preferred_element_type=f32)
            w = wd[2 * k + 1 - c, :, s].reshape(feats, half)
            acc += jnp.dot(theirs[k], w, preferred_element_type=f32)
        pre = jnp.maximum(hidden[:, cols].astype(f32), 0.0)
        out[:, cols] = (acc * 2.0 * pre).astype(bf16)


def grad_up_kernel(core, mine, theirs, inputs, out):
    c = core[0]
    right = inputs[...]
    for k in range(mine.shape[0]):
        g = jnp.dot(mine[k].T, right, preferred_element_type=f32)
        out[2 * k + c] = g.astype(bf16)
        g = jnp.dot(theirs[k].T, right, preferred_element_type=f32)
        out[2 * k + 1 - c] = g.astype(bf16)


def grad_input_kernel(core, mine, theirs, wu, out):
    c = core[0]
    acc = jnp.zeros(out.shape, f32)
    for k in range(mine.shape[0]):
        acc += jnp.dot(mine[k], wu[2 * k + c], preferred_element_type=f32)
        acc += jnp.dot(theirs[k], wu[2 * k + 1 - c], preferred_element_type=f32)
    out[...] = acc.astype(bf16)


def run(kernel, shape, *operands):
    scalar = pl.BlockSpec(memory_space=pltpu.SMEM)
    whole = pl.BlockSpec(memory_space=pltpu.VMEM)
    return pl.pallas_call(
        kernel,
        out_shape=jax.ShapeDtypeStruct(shape, bf16),
        in_specs=[scalar] + [whole] * (len(operands) - 1),
        out_specs=whole,
        name=kernel.__name__,
    )(*operands)


def on_device(inputs, hidden_pre, norm_input, out_gain, w_up, w_down, cotangent):
    nz, ny, ntp = (lax.axis_size(a) for a in ("z", "y", TP))
    toks, feats = inputs.shape
    hid = hidden_pre.shape[1]
    half = hid // 2
    width = feats * ntp
    scaled = (toks * nz * ny) ** (-0.5)
    core = lax.axis_index("c").astype(jnp.int32).reshape(1)

    normed = norm_input.astype(f32)
    upstream = cotangent.astype(f32)
    weighted = upstream * out_gain
    sums = jnp.stack([jnp.sum(normed * normed, axis=1), jnp.sum(weighted * normed, axis=1)])

    wd = w_down.T
    both = jnp.concatenate([wd[:, :half], wd[:, half:], w_up.T], axis=0)
    both = gather_directly(both, "y")
    wd_rows = 2 * wd.shape[0]
    wd = wd_y = both[:, :wd_rows].reshape(ny * wd_rows, half)
    wd = lax.all_gather(wd, "z", axis=0, tiled=True).reshape(nz, ny, 2, wd_rows // 2, half)
    wu = both[:, wd_rows:].reshape(hid, feats)

    sums = jnp.sum(gather_directly(after(sums, wd_y), TP), axis=0)
    inv_rms = lax.rsqrt(sums[0] / width + norm_eps)[:, None]
    cross_mean = (sums[1] / width)[:, None]
    d_out = (weighted * inv_rms - normed * inv_rms * inv_rms * inv_rms * cross_mean).astype(bf16)
    gain_part = jnp.sum(upstream * normed * inv_rms, axis=0) * scaled

    mine, theirs = gather_two_steps(d_out)
    d_pre = run(d_pre_kernel, (toks, hid), core, mine, theirs, wd, hidden_pre)
    wu = lax.all_gather(after(wu, mine), "z", axis=0, tiled=True).reshape(nz, hid, feats)

    mine, theirs = gather_two_steps(d_pre)
    g = run(grad_up_kernel, (ntp, hid, feats), core, mine, theirs, after(inputs, wu))
    g = lax.psum_scatter(g.reshape(nz * hid, feats), "z", scatter_dimension=0, tiled=True)
    grad_input = run(grad_input_kernel, (toks, feats), core, mine, theirs, wu)

    grad_gain = jnp.sum(gather_directly(after(gain_part, theirs), FS), axis=0)
    g = after(g, grad_gain)
    grad_up = (summed(exchange(g.reshape(ny, hid // ny, feats), "y")) * scaled).T
    return (grad_input, grad_up, grad_gain)


def solution(mesh):
    torus = Mesh(mesh.devices.reshape(8, 8, mesh.shape["tp"] // 2, 2), ("z", "y", "x", "c"))
    in_specs = (
        P(FS, TP),
        P(FS, TP),
        P(FS, TP),
        P(TP),
        P(TP, FS),
        P(TP, FS),
        P(FS, TP),
    )
    out_specs = (P(FS, TP), P(TP, FS), P(TP))
    return jax.shard_map(
        on_device, mesh=torus, in_specs=in_specs, out_specs=out_specs, check_vma=False
    )
```

```python
import jax
import jax.numpy as jnp
from jax import lax
from jax.experimental import pallas as pl
from jax.experimental.pallas import tpu as pltpu
from jax.sharding import Mesh
from jax.sharding import PartitionSpec as P

FS = ("z", "y")
TP = ("x", "c")
bf16 = jnp.bfloat16
f32 = jnp.float32
norm_eps = 1e-06


def exchange(chunks, axis):
    return lax.all_to_all(chunks, axis, 0, 0, tiled=True)


def gather_directly(value, axis):
    n = lax.axis_size(axis)
    return exchange(jnp.broadcast_to(value[None], (n, *value.shape)), axis)


def swapped(value):
    return lax.ppermute(value, "c", [(0, 1), (1, 0)])


def gather_two_steps(value):
    mine = gather_directly(value, "x")
    return mine, swapped(mine)


def after(value, earlier):
    return lax.optimization_barrier((value, earlier))[0]


def summed(parts):
    return jnp.sum(parts.astype(f32), axis=0)


def in_three(value):
    high = lax.reduce_precision(value, 8, 7)
    middle = lax.reduce_precision(value - high, 8, 7)
    return jnp.stack([high, middle, value - high - middle])


def grad_up_kernel(place, mine, theirs, wd, hidden, gain_rows, d_pre_out, g_out):
    c = place[0]
    chips, _, toks, feats = mine.shape
    half = wd.shape[-1]
    for s in range(2):
        cols = slice(s * half, (s + 1) * half)
        acc = jnp.zeros((toks, half), f32)
        for k in range(chips):
            w = wd[:, 2 * k + c, s].reshape(feats, half)
            acc += jnp.dot(mine[k, 0], w, preferred_element_type=f32)
            w = wd[:, 2 * k + 1 - c, s].reshape(feats, half)
            acc += jnp.dot(theirs[k, 0], w, preferred_element_type=f32)
        pre = jnp.maximum(hidden[:, cols].astype(f32), 0.0)
        d_pre_out[:, cols] = (acc * 2.0 * pre).astype(bf16)
    left = d_pre_out[...].T
    hid = hidden.shape[1]
    for k in range(chips):
        g = jnp.dot(left, mine[k, 1], preferred_element_type=f32)
        g_out[2 * k + c, :hid] = g.astype(bf16)
        g = jnp.dot(left, theirs[k, 1], preferred_element_type=f32)
        g_out[2 * k + 1 - c, :hid] = g.astype(bf16)
    for k in range(2 * chips):
        g_out[k, hid:] = gain_rows[...]


def grad_input_kernel(place, mine, theirs, *rest):
    *pieces, out, wu = rest
    c = place[0]
    ny = len(pieces)
    rows = pieces[0].shape[1]
    for d in range(ny):
        source = lax.rem(place[1] + ny - d, ny)
        start = pl.multiple_of(source * rows, rows)
        wu[:, pl.ds(start, rows), :] = pieces[d][...]
    acc = jnp.zeros(out.shape, f32)
    for k in range(mine.shape[0]):
        acc += jnp.dot(mine[k], wu[2 * k + c], preferred_element_type=f32)
        acc += jnp.dot(theirs[k], wu[2 * k + 1 - c], preferred_element_type=f32)
    out[...] = acc.astype(bf16)


def run(kernel, shapes, *operands, scratch=()):
    scalar = pl.BlockSpec(memory_space=pltpu.SMEM)
    whole = pl.BlockSpec(memory_space=pltpu.VMEM)
    return pl.pallas_call(
        kernel,
        out_shape=[jax.ShapeDtypeStruct(shape, bf16) for shape in shapes],
        in_specs=[scalar] + [whole] * (len(operands) - 1),
        out_specs=[whole] * len(shapes),
        scratch_shapes=[pltpu.VMEM(shape, bf16) for shape in scratch],
        name=kernel.__name__,
    )(*operands)


def on_device(inputs, hidden_pre, norm_input, out_gain, w_up, w_down, cotangent):
    nz, ny, ntp = (lax.axis_size(a) for a in ("z", "y", TP))
    toks, feats = inputs.shape
    hid = hidden_pre.shape[1]
    half = hid // 2
    width = feats * ntp
    scaled = (toks * nz * ny) ** (-0.5)
    place = jnp.stack([lax.axis_index("c"), lax.axis_index("y")]).astype(jnp.int32)
    swap = [(a * ntp + b, b * ntp + a) for a in range(nz) for b in range(ntp)]

    normed = norm_input.astype(f32)
    upstream = cotangent.astype(f32)
    weighted = upstream * out_gain
    sums = jnp.stack([jnp.sum(normed * normed, axis=1), jnp.sum(weighted * normed, axis=1)])

    wd = w_down.T
    both = jnp.concatenate([wd[:, :half], wd[:, half:], w_up.T], axis=0)
    both = gather_directly(both, "z")
    wd_rows = 2 * wd.shape[0]
    wd = wd_z = both[:, :wd_rows].reshape(nz * wd_rows, half)
    wd = lax.all_gather(wd, "y", axis=0, tiled=True)
    wd = wd.reshape(ny, nz, 2, wd_rows // 2, half)
    wu = both[:, wd_rows:]

    sums = jnp.sum(gather_directly(after(sums, wd_z), TP), axis=0)
    inv_rms = lax.rsqrt(sums[0] / width + norm_eps)[:, None]
    cross_mean = (sums[1] / width)[:, None]
    d_out = (weighted * inv_rms - normed * inv_rms * inv_rms * inv_rms * cross_mean).astype(bf16)
    gain_part = jnp.sum(upstream * normed * inv_rms, axis=0)

    mine, theirs = gather_two_steps(jnp.stack([d_out, inputs]))
    turn = (jnp.arange(nz) == lax.axis_index("z")).astype(f32)[:, None, None]
    gain_rows = (turn * in_three(gain_part)).reshape(3 * nz, feats).astype(bf16)
    d_pre, g = run(
        grad_up_kernel, [(toks, hid), (ntp, hid + 3 * nz, feats)],
        place, mine, theirs, wd, hidden_pre, gain_rows,
    )
    g = lax.psum_scatter(g.reshape(-1, feats), "z", scatter_dimension=0, tiled=True)

    wu = after(wu, d_pre)
    pieces = [wu]
    for d in range(1, ny):
        pieces.append(lax.ppermute(wu, "y", [(i, (i + d) % ny) for i in range(ny)]))
    mine = gather_directly(d_pre, "x")
    theirs = swapped(after(mine, pieces))
    [grad_input] = run(
        grad_input_kernel, [(toks, feats)], place, mine, theirs, *pieces,
        scratch=[(nz, hid, feats)],
    )

    rows = hid // ny
    gain = summed(g[hid:].reshape(nz, 3, feats))
    gain = in_three(jnp.sum(gain, axis=0)).astype(bf16)
    gain = jnp.broadcast_to(jnp.pad(gain, ((0, 5), (0, 0))), (ny, 8, feats))
    g = jnp.concatenate([g[:hid].reshape(ny, rows, feats), gain], axis=1)
    g = summed(exchange(g, "y")) * scaled
    grad_gain = jnp.sum(g[rows : rows + 3], axis=0)
    grad_up = lax.ppermute(g[:rows], ("z", "x", "c"), swap).T
    return (grad_input, grad_up, grad_gain)


def solution(mesh):
    torus = Mesh(mesh.devices.reshape(8, 8, mesh.shape["tp"] // 2, 2), ("z", "y", "x", "c"))
    in_specs = (
        P(FS, TP),
        P(FS, TP),
        P(FS, TP),
        P(TP),
        P(TP, FS),
        P(TP, FS),
        P(FS, TP),
    )
    out_specs = (P(FS, TP), P(TP, FS), P(TP))
    return jax.shard_map(
        on_device, mesh=torus, in_specs=in_specs, out_specs=out_specs, check_vma=False
    )
```

```python
import jax
import jax.numpy as jnp
from jax import lax
from jax.experimental import pallas as pl
from jax.experimental.pallas import tpu as pltpu
from jax.sharding import Mesh
from jax.sharding import PartitionSpec as P

FS = ("z", "y")
TP = ("x", "c")
bf16 = jnp.bfloat16
f32 = jnp.float32
norm_eps = 1e-06


def exchange(chunks, axis):
    return lax.all_to_all(chunks, axis, 0, 0, tiled=True)


def gather_directly(value, axis):
    n = lax.axis_size(axis)
    return exchange(jnp.broadcast_to(value[None], (n, *value.shape)), axis)


def shifted(value, axis, by):
    n = lax.axis_size(axis)
    return lax.ppermute(value, axis, [(i, (i + by) % n) for i in range(n)])


def swapped(value):
    return shifted(value, "c", 1)


def gather_two_steps(value):
    mine = gather_directly(value, "x")
    return mine, swapped(mine)


def after(value, earlier):
    return lax.optimization_barrier((value, earlier))[0]


def summed(parts):
    return jnp.sum(parts.astype(f32), axis=0)


def in_three(value):
    high = lax.reduce_precision(value, 8, 7)
    middle = lax.reduce_precision(value - high, 8, 7)
    return jnp.stack([high, middle, value - high - middle])


def grad_up_kernel(place, mine, theirs, wd, hidden, gain_rows, d_pre_out, g_out):
    c = place[0]
    chips, _, toks, feats = mine.shape
    half = wd.shape[-1]
    for s in range(2):
        cols = slice(s * half, (s + 1) * half)
        acc = jnp.zeros((toks, half), f32)
        for k in range(chips):
            w = wd[:, 2 * k + c, s].reshape(feats, half)
            acc += jnp.dot(mine[k, 0], w, preferred_element_type=f32)
            w = wd[:, 2 * k + 1 - c, s].reshape(feats, half)
            acc += jnp.dot(theirs[k, 0], w, preferred_element_type=f32)
        pre = jnp.maximum(hidden[:, cols].astype(f32), 0.0)
        d_pre_out[:, cols] = (acc * 2.0 * pre).astype(bf16)
    left = d_pre_out[...].T
    hid = hidden.shape[1]
    for k in range(chips):
        g = jnp.dot(left, mine[k, 1], preferred_element_type=f32)
        g_out[2 * k + c, :hid] = g.astype(bf16)
        g = jnp.dot(left, theirs[k, 1], preferred_element_type=f32)
        g_out[2 * k + 1 - c, :hid] = g.astype(bf16)
    for k in range(2 * chips):
        g_out[k, hid:] = gain_rows[...]


def grad_input_kernel(place, mine, theirs, *rest):
    *pieces, out, wu = rest
    c = place[0]
    ny = len(pieces)
    rows = pieces[0].shape[1]
    for d in range(ny):
        source = lax.rem(place[1] + ny - d, ny)
        start = pl.multiple_of(source * rows, rows)
        wu[:, pl.ds(start, rows), :] = pieces[d][...]
    acc = jnp.zeros(out.shape, f32)
    for k in range(mine.shape[0]):
        acc += jnp.dot(mine[k], wu[2 * k + c], preferred_element_type=f32)
        acc += jnp.dot(theirs[k], wu[2 * k + 1 - c], preferred_element_type=f32)
    out[...] = acc.astype(bf16)


def run(kernel, shapes, *operands, scratch=()):
    scalar = pl.BlockSpec(memory_space=pltpu.SMEM)
    whole = pl.BlockSpec(memory_space=pltpu.VMEM)
    return pl.pallas_call(
        kernel,
        out_shape=[jax.ShapeDtypeStruct(shape, bf16) for shape in shapes],
        in_specs=[scalar] + [whole] * (len(operands) - 1),
        out_specs=[whole] * len(shapes),
        scratch_shapes=[pltpu.VMEM(shape, bf16) for shape in scratch],
    )(*operands)


def one_device(inputs, hidden_pre, norm_input, out_gain, w_up, w_down, cotangent):
    nz, ny, ntp = (lax.axis_size(a) for a in ("z", "y", TP))
    toks, feats = inputs.shape
    hid = hidden_pre.shape[1]
    half = hid // 2
    width = feats * ntp
    scaled = (toks * nz * ny) ** (-0.5)
    place = jnp.stack([lax.axis_index("c"), lax.axis_index("y")]).astype(jnp.int32)
    swap = [(a * ntp + b, b * ntp + a) for a in range(nz) for b in range(ntp)]

    normed = norm_input.astype(f32)
    upstream = cotangent.astype(f32)
    weighted = upstream * out_gain
    sums = jnp.stack([jnp.sum(normed * normed, axis=1), jnp.sum(weighted * normed, axis=1)])

    wd = w_down.T
    both = jnp.concatenate([wd[:, :half], wd[:, half:], w_up.T], axis=0)
    both = gather_directly(both, "z")
    wd_rows = 2 * wd.shape[0]
    wd = wd_z = both[:, :wd_rows].reshape(nz * wd_rows, half)
    wd = lax.all_gather(wd, "y", axis=0, tiled=True)
    wd = wd.reshape(ny, nz, 2, wd_rows // 2, half)
    wu = both[:, wd_rows:]

    sums = gather_directly(after(sums, wd_z), TP)
    sums = jnp.sum(sums, axis=0)
    inv_rms = lax.rsqrt(sums[0] / width + norm_eps)[:, None]
    cross_mean = (sums[1] / width)[:, None]
    d_out = (weighted * inv_rms - normed * inv_rms * inv_rms * inv_rms * cross_mean).astype(bf16)
    gain_part = jnp.sum(upstream * normed * inv_rms, axis=0)

    mine, theirs = gather_two_steps(jnp.stack([d_out, inputs]))
    turn = (jnp.arange(nz) == lax.axis_index("z")).astype(f32)[:, None, None]
    gain_rows = (turn * in_three(gain_part)).reshape(3 * nz, feats).astype(bf16)
    d_pre, g = run(
        grad_up_kernel, [(toks, hid), (ntp, hid + 3 * nz, feats)],
        place, mine, theirs, wd, hidden_pre, gain_rows,
    )
    g = lax.psum_scatter(g.reshape(-1, feats), "z", scatter_dimension=0, tiled=True)

    wu = after(wu, d_pre)
    pieces = [wu] * ny
    for d in range(1, ny // 2 + 1):
        pieces[d] = shifted(pieces[d - 1], "y", 1)
        if ny - d > d:
            pieces[ny - d] = shifted(pieces[(ny - d + 1) % ny], "y", -1)
    mine = gather_directly(d_pre, "x")
    theirs = swapped(after(mine, pieces))
    [grad_input] = run(
        grad_input_kernel, [(toks, feats)], place, mine, theirs, *pieces,
        scratch=[(nz, hid, feats)],
    )

    rows = hid // ny
    gain = summed(g[hid:].reshape(nz, 3, feats))
    gain = in_three(jnp.sum(gain, axis=0)).astype(bf16)
    gain = jnp.broadcast_to(jnp.pad(gain, ((0, 5), (0, 0))), (ny, 8, feats))
    g = jnp.concatenate([g[:hid].reshape(ny, rows, feats), gain], axis=1)
    g = summed(exchange(g, "y")) * scaled
    grad_gain = jnp.sum(g[rows : rows + 3], axis=0)
    grad_up = lax.ppermute(g[:rows], ("z", "x", "c"), swap).T
    return (grad_input, grad_up, grad_gain)


def solution(mesh):
    torus = Mesh(mesh.devices.reshape(8, 8, mesh.shape["tp"] // 2, 2), ("z", "y", "x", "c"))
    in_specs = (
        P(FS, TP),
        P(FS, TP),
        P(FS, TP),
        P(TP),
        P(TP, FS),
        P(TP, FS),
        P(FS, TP),
    )
    out_specs = (P(FS, TP), P(TP, FS), P(TP))
    return jax.shard_map(
        one_device, mesh=torus, in_specs=in_specs, out_specs=out_specs, check_vma=False
    )
```

```python
import jax
import jax.numpy as jnp
from jax import lax
from jax.experimental import pallas as pl
from jax.experimental.pallas import tpu as pltpu
from jax.sharding import Mesh
from jax.sharding import PartitionSpec as P

FS = ("z", "y")
TP = ("x", "c")
bf16 = jnp.bfloat16
f32 = jnp.float32
norm_eps = 1e-06


def exchange(chunks, axis):
    return lax.all_to_all(chunks, axis, 0, 0, tiled=True)


def gather_directly(value, axis):
    n = lax.axis_size(axis)
    return exchange(jnp.broadcast_to(value[None], (n, *value.shape)), axis)


def shifted(value, axis, by):
    n = lax.axis_size(axis)
    return lax.ppermute(value, axis, [(i, (i + by) % n) for i in range(n)])


def swapped(value):
    return shifted(value, "c", 1)


def gather_two_steps(value):
    mine = gather_directly(value, "x")
    return mine, swapped(mine)


def after(value, earlier):
    return lax.optimization_barrier((value, earlier))[0]


def summed(parts):
    return jnp.sum(parts.astype(f32), axis=0)


def in_three(value):
    high = lax.reduce_precision(value, 8, 7)
    middle = lax.reduce_precision(value - high, 8, 7)
    return jnp.stack([high, middle, value - high - middle])


def grad_up_kernel(place, mine, theirs, wd, hidden, gain_rows, d_pre_out, g_out):
    c = place[0]
    chips, _, toks, feats = mine.shape
    half = wd.shape[-1]
    for s in range(2):
        cols = slice(s * half, (s + 1) * half)
        acc = jnp.zeros((toks, half), f32)
        for k in range(chips):
            w = wd[:, 2 * k + c, s].reshape(feats, half)
            acc += jnp.dot(mine[k, 0], w, preferred_element_type=f32)
            w = wd[:, 2 * k + 1 - c, s].reshape(feats, half)
            acc += jnp.dot(theirs[k, 0], w, preferred_element_type=f32)
        pre = jnp.maximum(hidden[:, cols].astype(f32), 0.0)
        d_pre_out[:, cols] = (acc * 2.0 * pre).astype(bf16)
    left = d_pre_out[...].T
    hid = hidden.shape[1]
    for k in range(chips):
        g = jnp.dot(left, mine[k, 1], preferred_element_type=f32)
        g_out[2 * k + c, :hid] = g.astype(bf16)
        g = jnp.dot(left, theirs[k, 1], preferred_element_type=f32)
        g_out[2 * k + 1 - c, :hid] = g.astype(bf16)
    for k in range(2 * chips):
        g_out[k, hid:] = gain_rows[...]


def grad_input_kernel(place, mine, theirs, *rest):
    *pieces, out, wu = rest
    c = place[0]
    ny = len(pieces)
    rows = pieces[0].shape[1]
    for d in range(ny):
        source = lax.rem(place[1] + ny - d, ny)
        start = pl.multiple_of(source * rows, rows)
        wu[:, pl.ds(start, rows), :] = pieces[d][...]
    acc = jnp.zeros(out.shape, f32)
    for k in range(mine.shape[0]):
        acc += jnp.dot(mine[k], wu[2 * k + c], preferred_element_type=f32)
        acc += jnp.dot(theirs[k], wu[2 * k + 1 - c], preferred_element_type=f32)
    out[...] = acc.astype(bf16)


def run(kernel, shapes, *operands, scratch=()):
    scalar = pl.BlockSpec(memory_space=pltpu.SMEM)
    whole = pl.BlockSpec(memory_space=pltpu.VMEM)
    return pl.pallas_call(
        kernel,
        out_shape=[jax.ShapeDtypeStruct(shape, bf16) for shape in shapes],
        in_specs=[scalar] + [whole] * (len(operands) - 1),
        out_specs=[whole] * len(shapes),
        scratch_shapes=[pltpu.VMEM(shape, bf16) for shape in scratch],
    )(*operands)


def one_device(inputs, hidden_pre, norm_input, out_gain, w_up, w_down, cotangent):
    nz, ny, ntp = (lax.axis_size(a) for a in ("z", "y", TP))
    toks, feats = inputs.shape
    hid = hidden_pre.shape[1]
    half = hid // 2
    width = feats * ntp
    scaled = (toks * nz * ny) ** (-0.5)
    place = jnp.stack([lax.axis_index("c"), lax.axis_index("y")]).astype(jnp.int32)
    swap = [(a * ntp + b, b * ntp + a) for a in range(nz) for b in range(ntp)]

    normed = norm_input.astype(f32)
    upstream = cotangent.astype(f32)
    weighted = upstream * out_gain
    sums = jnp.stack([jnp.sum(normed * normed, axis=1), jnp.sum(weighted * normed, axis=1)])

    wd = w_down.T
    both = jnp.concatenate([wd[:, :half], wd[:, half:], w_up.T], axis=0)
    both = gather_directly(both, "z")
    wd_rows = 2 * wd.shape[0]
    wd = wd_z = both[:, :wd_rows].reshape(nz * wd_rows, half)
    wd = lax.all_gather(wd, "y", axis=0, tiled=True)
    wd = wd.reshape(ny, nz, 2, wd_rows // 2, half)
    wu = both[:, wd_rows:]

    sums = gather_directly(after(sums, wd_z), TP)
    sums = jnp.sum(sums, axis=0)
    inv_rms = lax.rsqrt(sums[0] / width + norm_eps)[:, None]
    cross_mean = (sums[1] / width)[:, None]
    d_out = (weighted * inv_rms - normed * inv_rms * inv_rms * inv_rms * cross_mean).astype(bf16)
    gain_part = jnp.sum(upstream * normed * inv_rms, axis=0)

    mine, theirs = gather_two_steps(jnp.stack([d_out, inputs]))
    turn = (jnp.arange(nz) == lax.axis_index("z")).astype(f32)[:, None, None]
    gain_rows = (turn * in_three(gain_part)).reshape(3 * nz, feats).astype(bf16)
    d_pre, g = run(
        grad_up_kernel, [(toks, hid), (ntp, hid + 3 * nz, feats)],
        place, mine, theirs, wd, hidden_pre, gain_rows,
    )
    g = lax.psum_scatter(g.reshape(-1, feats), "z", scatter_dimension=0, tiled=True)

    wu = after(wu, d_pre)
    pieces = [wu] * ny
    for d in range(1, ny // 2):
        pieces[d] = shifted(pieces[d - 1], "y", 1)
        pieces[ny - d] = shifted(pieces[(ny - d + 1) % ny], "y", -1)
    mine = gather_directly(d_pre, "x")
    theirs = swapped(after(mine, pieces))
    rows = hid // ny
    gain = summed(g[hid:].reshape(nz, 3, feats))
    gain = in_three(jnp.sum(gain, axis=0)).astype(bf16)
    gain = jnp.broadcast_to(jnp.pad(gain, ((0, 5), (0, 0))), (ny, 8, feats))
    g = jnp.concatenate([g[:hid].reshape(ny, rows, feats), gain], axis=1)
    last = after(pieces[ny // 2 - 1], g)
    g = summed(exchange(g, "y")) * scaled
    grad_gain = jnp.sum(g[rows : rows + 3], axis=0)
    grad_up = lax.ppermute(g[:rows], ("z", "x", "c"), swap).T

    pieces[ny // 2] = shifted(last, "y", 1)
    [grad_input] = run(
        grad_input_kernel, [(toks, feats)], place, mine, theirs, *pieces,
        scratch=[(nz, hid, feats)],
    )
    return (grad_input, grad_up, grad_gain)


def solution(mesh):
    torus = Mesh(mesh.devices.reshape(8, 8, mesh.shape["tp"] // 2, 2), ("z", "y", "x", "c"))
    in_specs = (
        P(FS, TP),
        P(FS, TP),
        P(FS, TP),
        P(TP),
        P(TP, FS),
        P(TP, FS),
        P(FS, TP),
    )
    out_specs = (P(FS, TP), P(TP, FS), P(TP))
    return jax.shard_map(
        one_device, mesh=torus, in_specs=in_specs, out_specs=out_specs, check_vma=False
    )
```

```python
import jax
import jax.numpy as jnp
from jax import lax
from jax.experimental import pallas as pl
from jax.experimental.pallas import tpu as pltpu
from jax.sharding import Mesh
from jax.sharding import PartitionSpec as P

FS = ("z", "y")
TP = ("x", "c")
bf16 = jnp.bfloat16
f32 = jnp.float32
norm_eps = 1e-06


def exchange(chunks, axis):
    return lax.all_to_all(chunks, axis, 0, 0, tiled=True)


def gather_directly(value, axis):
    n = lax.axis_size(axis)
    return exchange(jnp.broadcast_to(value[None], (n, *value.shape)), axis)


def shifted(value, axis, by):
    n = lax.axis_size(axis)
    return lax.ppermute(value, axis, [(i, (i + by) % n) for i in range(n)])


def swapped(value):
    return shifted(value, "c", 1)


def after(value, earlier):
    return lax.optimization_barrier((value, earlier))[0]


def summed(parts):
    return jnp.sum(parts.astype(f32), axis=0)


def in_three(value):
    high = lax.reduce_precision(value, 8, 7)
    middle = lax.reduce_precision(value - high, 8, 7)
    return jnp.stack([high, middle, value - high - middle])


def grad_up_kernel(place, mine, theirs, wd, hidden, gain_rows, d_pre_out, g_out):
    c = place[0]
    chips, _, toks, feats = mine.shape
    half = wd.shape[-1]
    for s in range(2):
        cols = slice(s * half, (s + 1) * half)
        acc = jnp.zeros((toks, half), f32)
        for k in range(chips):
            w = wd[:, 2 * k + c, s].reshape(feats, half)
            acc += jnp.dot(mine[k, 0], w, preferred_element_type=f32)
            w = wd[:, 2 * k + 1 - c, s].reshape(feats, half)
            acc += jnp.dot(theirs[k, 0], w, preferred_element_type=f32)
        pre = jnp.maximum(hidden[:, cols].astype(f32), 0.0)
        d_pre_out[:, cols] = (acc * 2.0 * pre).astype(bf16)
    left = d_pre_out[...].T
    hid = hidden.shape[1]
    for k in range(chips):
        g = jnp.dot(left, mine[k, 1], preferred_element_type=f32)
        g_out[2 * k + c, :hid] = g.astype(bf16)
        g = jnp.dot(left, theirs[k, 1], preferred_element_type=f32)
        g_out[2 * k + 1 - c, :hid] = g.astype(bf16)
    for k in range(2 * chips):
        g_out[k, hid:] = gain_rows[...]


def grad_input_kernel(place, mine, theirs, *rest):
    *pieces, out, wu = rest
    c = place[0]
    ny = len(pieces)
    rows = pieces[0].shape[1]
    for d in range(ny):
        source = lax.rem(place[1] + ny - d, ny)
        start = pl.multiple_of(source * rows, rows)
        wu[:, pl.ds(start, rows), :] = pieces[d][...]
    acc = jnp.zeros(out.shape, f32)
    for k in range(mine.shape[0]):
        acc += jnp.dot(mine[k], wu[2 * k + c], preferred_element_type=f32)
        acc += jnp.dot(theirs[k], wu[2 * k + 1 - c], preferred_element_type=f32)
    out[...] = acc.astype(bf16)


def run(kernel, shapes, *operands, scratch=()):
    scalar = pl.BlockSpec(memory_space=pltpu.SMEM)
    whole = pl.BlockSpec(memory_space=pltpu.VMEM)
    return pl.pallas_call(
        kernel,
        out_shape=[jax.ShapeDtypeStruct(shape, bf16) for shape in shapes],
        in_specs=[scalar] + [whole] * (len(operands) - 1),
        out_specs=[whole] * len(shapes),
        scratch_shapes=[pltpu.VMEM(shape, bf16) for shape in scratch],
    )(*operands)


def one_device(inputs, hidden_pre, norm_input, out_gain, w_up, w_down, cotangent):
    nz, ny, ntp = (lax.axis_size(a) for a in ("z", "y", TP))
    toks, feats = inputs.shape
    hid = hidden_pre.shape[1]
    half = hid // 2
    width = feats * ntp
    scaled = (toks * nz * ny) ** (-0.5)
    place = jnp.stack([lax.axis_index("c"), lax.axis_index("y")]).astype(jnp.int32)
    swap = [(a * ntp + b, b * ntp + a) for a in range(nz) for b in range(ntp)]

    normed = norm_input.astype(f32)
    upstream = cotangent.astype(f32)
    weighted = upstream * out_gain
    sums = jnp.stack([jnp.sum(normed * normed, axis=1), jnp.sum(weighted * normed, axis=1)])

    wd = w_down.T
    both = jnp.concatenate([wd[:, :half], wd[:, half:], w_up.T], axis=0)
    both = gather_directly(both, "z")
    wd_rows = 2 * wd.shape[0]
    wd = wd_z = both[:, :wd_rows].reshape(nz * wd_rows, half)
    wd = lax.all_gather(wd, "y", axis=0, tiled=True)
    wd = wd.reshape(ny, nz, 2, wd_rows // 2, half)
    wu = both[:, wd_rows:]

    sums = gather_directly(after(sums, wd_z), TP)
    sums = jnp.sum(sums, axis=0)
    inv_rms = lax.rsqrt(sums[0] / width + norm_eps)[:, None]
    cross_mean = (sums[1] / width)[:, None]
    d_out = (weighted * inv_rms - normed * inv_rms * inv_rms * inv_rms * cross_mean).astype(bf16)
    gain_part = jnp.sum(upstream * normed * inv_rms, axis=0)

    wu = after(wu, inv_rms)
    pieces = [wu] * ny
    pieces[1], pieces[ny - 1] = shifted(wu, "y", 1), shifted(wu, "y", -1)
    mine = gather_directly(jnp.stack([d_out, inputs]), "x")
    theirs = swapped(after(mine, (pieces[1], pieces[ny - 1])))
    turn = (jnp.arange(nz) == lax.axis_index("z")).astype(f32)[:, None, None]
    gain_rows = (turn * in_three(gain_part)).reshape(3 * nz, feats).astype(bf16)
    d_pre, g = run(
        grad_up_kernel, [(toks, hid), (ntp, hid + 3 * nz, feats)],
        place, mine, theirs, wd, hidden_pre, gain_rows,
    )
    g = lax.psum_scatter(g.reshape(-1, feats), "z", scatter_dimension=0, tiled=True)

    pieces[1] = after(pieces[1], d_pre)
    pieces[ny - 1] = after(pieces[ny - 1], d_pre)
    for d in range(2, ny // 2 + 1):
        pieces[d] = shifted(pieces[d - 1], "y", 1)
        if ny - d > d:
            pieces[ny - d] = shifted(pieces[(ny - d + 1) % ny], "y", -1)
    mine = gather_directly(d_pre, "x")
    theirs = swapped(after(mine, pieces))
    [grad_input] = run(
        grad_input_kernel, [(toks, feats)], place, mine, theirs, *pieces,
        scratch=[(nz, hid, feats)],
    )

    rows = hid // ny
    gain = summed(g[hid:].reshape(nz, 3, feats))
    gain = in_three(jnp.sum(gain, axis=0)).astype(bf16)
    gain = jnp.broadcast_to(jnp.pad(gain, ((0, 5), (0, 0))), (ny, 8, feats))
    g = jnp.concatenate([g[:hid].reshape(ny, rows, feats), gain], axis=1)
    g = summed(exchange(g, "y")) * scaled
    grad_gain = jnp.sum(g[rows : rows + 3], axis=0)
    grad_up = lax.ppermute(g[:rows], ("z", "x", "c"), swap).T
    return (grad_input, grad_up, grad_gain)


def solution(mesh):
    torus = Mesh(mesh.devices.reshape(8, 8, mesh.shape["tp"] // 2, 2), ("z", "y", "x", "c"))
    in_specs = (
        P(FS, TP),
        P(FS, TP),
        P(FS, TP),
        P(TP),
        P(TP, FS),
        P(TP, FS),
        P(FS, TP),
    )
    out_specs = (P(FS, TP), P(TP, FS), P(TP))
    return jax.shard_map(
        one_device, mesh=torus, in_specs=in_specs, out_specs=out_specs, check_vma=False
    )
```

```python
import jax
import jax.numpy as jnp
from jax import lax
from jax.experimental import pallas as pl
from jax.experimental.pallas import tpu as pltpu
from jax.sharding import Mesh
from jax.sharding import PartitionSpec as P

FS = ("z", "y")
TP = ("x", "c")
bf16 = jnp.bfloat16
f32 = jnp.float32
norm_eps = 1e-06


def exchange(chunks, axis):
    return lax.all_to_all(chunks, axis, 0, 0, tiled=True)


def gather_directly(value, axis):
    n = lax.axis_size(axis)
    return exchange(jnp.broadcast_to(value[None], (n, *value.shape)), axis)


def shifted(value, axis, by):
    n = lax.axis_size(axis)
    return lax.ppermute(value, axis, [(i, (i + by) % n) for i in range(n)])


def swapped(value):
    return shifted(value, "c", 1)


def pairwise(value, axes):
    for axis in reversed(axes):
        n = lax.axis_size(axis)
        step = 1
        while step < n:
            value = value + lax.ppermute(value, axis, [(i, i ^ step) for i in range(n)])
            step *= 2
    return value


def after(value, earlier):
    return lax.optimization_barrier((value, earlier))[0]


def summed(parts):
    return jnp.sum(parts.astype(f32), axis=0)


def in_three(value):
    high = lax.reduce_precision(value, 8, 7)
    middle = lax.reduce_precision(value - high, 8, 7)
    return jnp.stack([high, middle, value - high - middle])


def grad_up_kernel(place, mine, theirs, wd, hidden, gain_rows, d_pre_out, g_out):
    c = place[0]
    chips, _, toks, feats = mine.shape
    half = wd.shape[-1]
    for s in range(2):
        cols = slice(s * half, (s + 1) * half)
        acc = jnp.zeros((toks, half), f32)
        for k in range(chips):
            w = wd[:, 2 * k + c, s].reshape(feats, half)
            acc += jnp.dot(mine[k, 0], w, preferred_element_type=f32)
            w = wd[:, 2 * k + 1 - c, s].reshape(feats, half)
            acc += jnp.dot(theirs[k, 0], w, preferred_element_type=f32)
        pre = jnp.maximum(hidden[:, cols].astype(f32), 0.0)
        d_pre_out[:, cols] = (acc * 2.0 * pre).astype(bf16)
    left = d_pre_out[...].T
    hid = hidden.shape[1]
    for k in range(chips):
        g = jnp.dot(left, mine[k, 1], preferred_element_type=f32)
        g_out[2 * k + c, :hid] = g.astype(bf16)
        g = jnp.dot(left, theirs[k, 1], preferred_element_type=f32)
        g_out[2 * k + 1 - c, :hid] = g.astype(bf16)
    for k in range(2 * chips):
        g_out[k, hid:] = gain_rows[...]


def grad_input_kernel(place, mine, theirs, *rest):
    *pieces, out, wu = rest
    c = place[0]
    ny = len(pieces)
    rows = pieces[0].shape[1]
    for d in range(ny):
        source = lax.rem(place[1] + ny - d, ny)
        start = pl.multiple_of(source * rows, rows)
        wu[:, pl.ds(start, rows), :] = pieces[d][...]
    acc = jnp.zeros(out.shape, f32)
    for k in range(mine.shape[0]):
        acc += jnp.dot(mine[k], wu[2 * k + c], preferred_element_type=f32)
        acc += jnp.dot(theirs[k], wu[2 * k + 1 - c], preferred_element_type=f32)
    out[...] = acc.astype(bf16)


def run(kernel, shapes, *operands, scratch=()):
    scalar = pl.BlockSpec(memory_space=pltpu.SMEM)
    whole = pl.BlockSpec(memory_space=pltpu.VMEM)
    return pl.pallas_call(
        kernel,
        out_shape=[jax.ShapeDtypeStruct(shape, bf16) for shape in shapes],
        in_specs=[scalar] + [whole] * (len(operands) - 1),
        out_specs=[whole] * len(shapes),
        scratch_shapes=[pltpu.VMEM(shape, bf16) for shape in scratch],
    )(*operands)


def one_device(inputs, hidden_pre, norm_input, out_gain, w_up, w_down, cotangent):
    nz, ny, ntp = (lax.axis_size(a) for a in ("z", "y", TP))
    toks, feats = inputs.shape
    hid = hidden_pre.shape[1]
    half = hid // 2
    width = feats * ntp
    scaled = (toks * nz * ny) ** (-0.5)
    place = jnp.stack([lax.axis_index("c"), lax.axis_index("y")]).astype(jnp.int32)
    swap = [(a * ntp + b, b * ntp + a) for a in range(nz) for b in range(ntp)]

    normed = norm_input.astype(f32)
    upstream = cotangent.astype(f32)
    weighted = upstream * out_gain
    sums = jnp.stack([jnp.sum(normed * normed, axis=1), jnp.sum(weighted * normed, axis=1)])

    wd = w_down.T
    both = jnp.concatenate([wd[:, :half], wd[:, half:], w_up.T], axis=0)
    both = gather_directly(both, "z")
    wd_rows = 2 * wd.shape[0]
    wd = both[:, :wd_rows].reshape(nz * wd_rows, half)
    wd = lax.all_gather(wd, "y", axis=0, tiled=True)
    wd = wd.reshape(ny, nz, 2, wd_rows // 2, half)
    wu = both[:, wd_rows:]

    sums = pairwise(sums, TP)
    inv_rms = lax.rsqrt(sums[0] / width + norm_eps)[:, None]
    cross_mean = (sums[1] / width)[:, None]
    d_out = (weighted * inv_rms - normed * inv_rms * inv_rms * inv_rms * cross_mean).astype(bf16)
    gain_part = jnp.sum(upstream * normed * inv_rms, axis=0)

    wu = after(wu, inv_rms)
    pieces = [wu] * ny
    pieces[1], pieces[ny - 1] = shifted(wu, "y", 1), shifted(wu, "y", -1)
    mine = gather_directly(jnp.stack([d_out, inputs]), "x")
    theirs = swapped(after(mine, (pieces[1], pieces[ny - 1])))
    turn = (jnp.arange(nz) == lax.axis_index("z")).astype(f32)[:, None, None]
    gain_rows = (turn * in_three(gain_part)).reshape(3 * nz, feats).astype(bf16)
    d_pre, g = run(
        grad_up_kernel, [(toks, hid), (ntp, hid + 3 * nz, feats)],
        place, mine, theirs, wd, hidden_pre, gain_rows,
    )
    g = lax.psum_scatter(g.reshape(-1, feats), "z", scatter_dimension=0, tiled=True)

    pieces[1] = after(pieces[1], d_pre)
    pieces[ny - 1] = after(pieces[ny - 1], d_pre)
    for d in range(2, ny // 2 + 1):
        pieces[d] = shifted(pieces[d - 1], "y", 1)
        if ny - d > d:
            pieces[ny - d] = shifted(pieces[(ny - d + 1) % ny], "y", -1)
    mine = gather_directly(d_pre, "x")
    theirs = swapped(after(mine, pieces))
    [grad_input] = run(
        grad_input_kernel, [(toks, feats)], place, mine, theirs, *pieces,
        scratch=[(nz, hid, feats)],
    )

    rows = hid // ny
    gain = summed(g[hid:].reshape(nz, 3, feats))
    gain = in_three(jnp.sum(gain, axis=0)).astype(bf16)
    gain = jnp.broadcast_to(jnp.pad(gain, ((0, 5), (0, 0))), (ny, 8, feats))
    g = jnp.concatenate([g[:hid].reshape(ny, rows, feats), gain], axis=1)
    g = summed(exchange(g, "y")) * scaled
    grad_gain = jnp.sum(g[rows : rows + 3], axis=0)
    grad_up = lax.ppermute(g[:rows], ("z", "x", "c"), swap).T
    return (grad_input, grad_up, grad_gain)


def solution(mesh):
    torus = Mesh(mesh.devices.reshape(8, 8, mesh.shape["tp"] // 2, 2), ("z", "y", "x", "c"))
    in_specs = (
        P(FS, TP),
        P(FS, TP),
        P(FS, TP),
        P(TP),
        P(TP, FS),
        P(TP, FS),
        P(FS, TP),
    )
    out_specs = (P(FS, TP), P(TP, FS), P(TP))
    return jax.shard_map(
        one_device, mesh=torus, in_specs=in_specs, out_specs=out_specs, check_vma=False
    )
```

```python
import jax
import jax.numpy as jnp
from jax import lax
from jax.experimental import pallas as pl
from jax.experimental.pallas import tpu as pltpu
from jax.sharding import Mesh
from jax.sharding import PartitionSpec as P

FS = ("z", "y")
TP = ("x", "c")
bf16 = jnp.bfloat16
f32 = jnp.float32
norm_eps = 1e-06


def exchange(chunks, axis):
    return lax.all_to_all(chunks, axis, 0, 0, tiled=True)


def gather_directly(value, axis):
    n = lax.axis_size(axis)
    return exchange(jnp.broadcast_to(value[None], (n, *value.shape)), axis)


def shifted(value, axis, by):
    n = lax.axis_size(axis)
    return lax.ppermute(value, axis, [(i, (i + by) % n) for i in range(n)])


def swapped(value):
    return shifted(value, "c", 1)


def pairwise(value, axes):
    for axis in reversed(axes):
        n = lax.axis_size(axis)
        step = 1
        while step < n:
            value = value + lax.ppermute(value, axis, [(i, i ^ step) for i in range(n)])
            step *= 2
    return value


def after(value, earlier):
    return lax.optimization_barrier((value, earlier))[0]


def summed(parts):
    return jnp.sum(parts.astype(f32), axis=0)


def in_three(value):
    high = lax.reduce_precision(value, 8, 7)
    middle = lax.reduce_precision(value - high, 8, 7)
    return jnp.stack([high, middle, value - high - middle])


def grad_up_kernel(place, mine, theirs, wd, hidden, gain_rows, d_pre_out, g_out):
    c = place[0]
    chips, _, toks, feats = mine.shape
    half = wd.shape[-1]
    for s in range(2):
        cols = slice(s * half, (s + 1) * half)
        acc = jnp.zeros((toks, half), f32)
        for k in range(chips):
            w = wd[:, 2 * k + c, s].reshape(feats, half)
            acc += jnp.dot(mine[k, 0], w, preferred_element_type=f32)
            w = wd[:, 2 * k + 1 - c, s].reshape(feats, half)
            acc += jnp.dot(theirs[k, 0], w, preferred_element_type=f32)
        pre = jnp.maximum(hidden[:, cols].astype(f32), 0.0)
        d_pre_out[:, cols] = (acc * 2.0 * pre).astype(bf16)
    left = d_pre_out[...].T
    hid = hidden.shape[1]
    for k in range(chips):
        g = jnp.dot(left, mine[k, 1], preferred_element_type=f32)
        g_out[2 * k + c, :hid] = g.astype(bf16)
        g = jnp.dot(left, theirs[k, 1], preferred_element_type=f32)
        g_out[2 * k + 1 - c, :hid] = g.astype(bf16)
    for k in range(2 * chips):
        g_out[k, hid:] = gain_rows[...]


def grad_input_kernel(place, mine, theirs, *rest):
    *pieces, out, wu = rest
    c = place[0]
    ny = len(pieces)
    rows = pieces[0].shape[1]
    for d in range(ny):
        source = lax.rem(place[1] + ny - d, ny)
        start = pl.multiple_of(source * rows, rows)
        wu[:, pl.ds(start, rows), :] = pieces[d][...]
    acc = jnp.zeros(out.shape, f32)
    for k in range(mine.shape[0]):
        acc += jnp.dot(mine[k], wu[2 * k + c], preferred_element_type=f32)
        acc += jnp.dot(theirs[k], wu[2 * k + 1 - c], preferred_element_type=f32)
    out[...] = acc.astype(bf16)


def run(kernel, shapes, *operands, scratch=()):
    scalar = pl.BlockSpec(memory_space=pltpu.SMEM)
    whole = pl.BlockSpec(memory_space=pltpu.VMEM)
    return pl.pallas_call(
        kernel,
        out_shape=[jax.ShapeDtypeStruct(shape, bf16) for shape in shapes],
        in_specs=[scalar] + [whole] * (len(operands) - 1),
        out_specs=[whole] * len(shapes),
        scratch_shapes=[pltpu.VMEM(shape, bf16) for shape in scratch],
    )(*operands)


def one_device(inputs, hidden_pre, norm_input, out_gain, w_up, w_down, cotangent):
    nz, ny, ntp = (lax.axis_size(a) for a in ("z", "y", TP))
    toks, feats = inputs.shape
    hid = hidden_pre.shape[1]
    half = hid // 2
    width = feats * ntp
    scaled = (toks * nz * ny) ** (-0.5)
    place = jnp.stack([lax.axis_index("c"), lax.axis_index("y")]).astype(jnp.int32)
    swap = [(a * ntp + b, b * ntp + a) for a in range(nz) for b in range(ntp)]

    normed = norm_input.astype(f32)
    upstream = cotangent.astype(f32)
    weighted = upstream * out_gain
    sums = jnp.stack([jnp.sum(normed * normed, axis=1), jnp.sum(weighted * normed, axis=1)])

    wd = w_down.T
    both = jnp.concatenate([wd[:, :half], wd[:, half:], w_up.T], axis=0)
    both = gather_directly(both, "z")
    wd_rows = 2 * wd.shape[0]
    wd = both[:, :wd_rows].reshape(nz * wd_rows, half)
    wd = lax.all_gather(wd, "y", axis=0, tiled=True)
    wd = wd.reshape(ny, nz, 2, wd_rows // 2, half)
    wu = both[:, wd_rows:]

    sums = pairwise(sums, TP)
    inv_rms = lax.rsqrt(sums[0] / width + norm_eps)[:, None]
    cross_mean = (sums[1] / width)[:, None]
    d_out = (weighted * inv_rms - normed * inv_rms * inv_rms * inv_rms * cross_mean).astype(bf16)
    gain_part = jnp.sum(upstream * normed * inv_rms, axis=0)

    wu = after(wu, inv_rms)
    pieces = [wu] * ny
    pieces[1] = shifted(wu, "y", 1)
    mine = gather_directly(jnp.stack([d_out, inputs]), "x")
    theirs = swapped(after(mine, pieces[1]))
    turn = (jnp.arange(nz) == lax.axis_index("z")).astype(f32)[:, None, None]
    gain_rows = (turn * in_three(gain_part)).reshape(3 * nz, feats).astype(bf16)
    d_pre, g = run(
        grad_up_kernel, [(toks, hid), (ntp, hid + 3 * nz, feats)],
        place, mine, theirs, wd, hidden_pre, gain_rows,
    )
    g = lax.psum_scatter(g.reshape(-1, feats), "z", scatter_dimension=0, tiled=True)

    pieces[1], left = after(pieces[1], d_pre), after(wu, d_pre)
    for d in range(1, ny // 2):
        pieces[d + 1] = shifted(pieces[d], "y", 1)
        pieces[ny - d] = left = shifted(left, "y", -1)
    mine = gather_directly(d_pre, "x")
    theirs = swapped(after(mine, pieces))
    [grad_input] = run(
        grad_input_kernel, [(toks, feats)], place, mine, theirs, *pieces,
        scratch=[(nz, hid, feats)],
    )

    rows = hid // ny
    gain = summed(g[hid:].reshape(nz, 3, feats))
    gain = in_three(jnp.sum(gain, axis=0)).astype(bf16)
    gain = jnp.broadcast_to(jnp.pad(gain, ((0, 5), (0, 0))), (ny, 8, feats))
    g = jnp.concatenate([g[:hid].reshape(ny, rows, feats), gain], axis=1)
    g = summed(exchange(g, "y")) * scaled
    grad_gain = jnp.sum(g[rows : rows + 3], axis=0)
    grad_up = lax.ppermute(g[:rows], ("z", "x", "c"), swap).T
    return (grad_input, grad_up, grad_gain)


def solution(mesh):
    torus = Mesh(mesh.devices.reshape(8, 8, mesh.shape["tp"] // 2, 2), ("z", "y", "x", "c"))
    in_specs = (
        P(FS, TP),
        P(FS, TP),
        P(FS, TP),
        P(TP),
        P(TP, FS),
        P(TP, FS),
        P(FS, TP),
    )
    out_specs = (P(FS, TP), P(TP, FS), P(TP))
    return jax.shard_map(
        one_device, mesh=torus, in_specs=in_specs, out_specs=out_specs, check_vma=False
    )
```

```python
import jax
import jax.numpy as jnp
from jax import lax
from jax.experimental import pallas as pl
from jax.experimental.pallas import tpu as pltpu
from jax.sharding import Mesh
from jax.sharding import PartitionSpec as P

FS = ("z", "y")
TP = ("x", "c")
bf16 = jnp.bfloat16
f32 = jnp.float32
norm_eps = 1e-06


def exchange(chunks, axis):
    return lax.all_to_all(chunks, axis, 0, 0, tiled=True)


def gather_directly(value, axis):
    n = lax.axis_size(axis)
    return exchange(jnp.broadcast_to(value[None], (n, *value.shape)), axis)


def shifted(value, axis, by):
    n = lax.axis_size(axis)
    return lax.ppermute(value, axis, [(i, (i + by) % n) for i in range(n)])


def swapped(value):
    return shifted(value, "c", 1)


def pairwise(value, axes):
    for axis in reversed(axes):
        n = lax.axis_size(axis)
        step = 1
        while step < n:
            value = value + lax.ppermute(value, axis, [(i, i ^ step) for i in range(n)])
            step *= 2
    return value


def after(value, earlier):
    return lax.optimization_barrier((value, earlier))[0]


def summed(parts):
    return jnp.sum(parts.astype(f32), axis=0)


def spread_kernel(wd, wu, out):
    rows, half = wd.shape[0], wd.shape[1] // 2
    for k in range(out.shape[0]):
        out[k, :rows] = wd[:, :half]
        out[k, rows : 2 * rows] = wd[:, half:]
        out[k, 2 * rows :] = wu[...]


def in_three(value):
    high = lax.reduce_precision(value, 8, 7)
    middle = lax.reduce_precision(value - high, 8, 7)
    return jnp.stack([high, middle, value - high - middle])


def grad_up_kernel(place, mine, theirs, wd, hidden, gain_rows, d_pre_out, g_out):
    c = place[0]
    chips, _, toks, feats = mine.shape
    half = wd.shape[-1]
    for s in range(2):
        cols = slice(s * half, (s + 1) * half)
        acc = jnp.zeros((toks, half), f32)
        for k in range(chips):
            w = wd[:, 2 * k + c, s].reshape(feats, half)
            acc += jnp.dot(mine[k, 0], w, preferred_element_type=f32)
            w = wd[:, 2 * k + 1 - c, s].reshape(feats, half)
            acc += jnp.dot(theirs[k, 0], w, preferred_element_type=f32)
        pre = jnp.maximum(hidden[:, cols].astype(f32), 0.0)
        d_pre_out[:, cols] = (acc * 2.0 * pre).astype(bf16)
    left = d_pre_out[...].T
    hid = hidden.shape[1]
    for k in range(chips):
        g = jnp.dot(left, mine[k, 1], preferred_element_type=f32)
        g_out[2 * k + c, :hid] = g.astype(bf16)
        g = jnp.dot(left, theirs[k, 1], preferred_element_type=f32)
        g_out[2 * k + 1 - c, :hid] = g.astype(bf16)
    for k in range(2 * chips):
        g_out[k, hid:] = gain_rows[...]


def grad_input_kernel(place, mine, theirs, *rest):
    *pieces, out, wu = rest
    c = place[0]
    ny = len(pieces)
    rows = pieces[0].shape[1]
    for d in range(ny):
        source = lax.rem(place[1] + ny - d, ny)
        start = pl.multiple_of(source * rows, rows)
        wu[:, pl.ds(start, rows), :] = pieces[d][...]
    acc = jnp.zeros(out.shape, f32)
    for k in range(mine.shape[0]):
        acc += jnp.dot(mine[k], wu[2 * k + c], preferred_element_type=f32)
        acc += jnp.dot(theirs[k], wu[2 * k + 1 - c], preferred_element_type=f32)
    out[...] = acc.astype(bf16)


def run(kernel, shapes, *operands, scratch=()):
    scalar = pl.BlockSpec(memory_space=pltpu.SMEM)
    whole = pl.BlockSpec(memory_space=pltpu.VMEM)
    return pl.pallas_call(
        kernel,
        out_shape=[jax.ShapeDtypeStruct(shape, bf16) for shape in shapes],
        in_specs=[scalar] + [whole] * (len(operands) - 1),
        out_specs=[whole] * len(shapes),
        scratch_shapes=[pltpu.VMEM(shape, bf16) for shape in scratch],
    )(*operands)


def one_device(inputs, hidden_pre, norm_input, out_gain, w_up, w_down, cotangent):
    nz, ny, ntp = (lax.axis_size(a) for a in ("z", "y", TP))
    toks, feats = inputs.shape
    hid = hidden_pre.shape[1]
    half = hid // 2
    width = feats * ntp
    scaled = (toks * nz * ny) ** (-0.5)
    place = jnp.stack([lax.axis_index("c"), lax.axis_index("y")]).astype(jnp.int32)
    swap = [(a * ntp + b, b * ntp + a) for a in range(nz) for b in range(ntp)]

    normed = norm_input.astype(f32)
    upstream = cotangent.astype(f32)
    weighted = upstream * out_gain
    sums = jnp.stack([jnp.sum(normed * normed, axis=1), jnp.sum(weighted * normed, axis=1)])

    wd = w_down.T
    rows = 2 * wd.shape[0] + w_up.shape[1]
    both = pl.pallas_call(
        spread_kernel,
        out_shape=jax.ShapeDtypeStruct((nz, rows, feats), bf16),
        name="spread_kernel",
    )(wd, w_up.T)
    both = exchange(both, "z")
    wd_rows = 2 * wd.shape[0]
    wd = both[:, :wd_rows].reshape(nz * wd_rows, half)
    wd = lax.all_gather(wd, "y", axis=0, tiled=True)
    wd = wd.reshape(ny, nz, 2, wd_rows // 2, half)
    wu = both[:, wd_rows:]

    sums = pairwise(sums, TP)
    inv_rms = lax.rsqrt(sums[0] / width + norm_eps)[:, None]
    cross_mean = (sums[1] / width)[:, None]
    d_out = (weighted * inv_rms - normed * inv_rms * inv_rms * inv_rms * cross_mean).astype(bf16)
    gain_part = jnp.sum(upstream * normed * inv_rms, axis=0)

    wu = after(wu, inv_rms)
    pieces = [wu] * ny
    pieces[1] = shifted(wu, "y", 1)
    mine = gather_directly(jnp.stack([d_out, inputs]), "x")
    theirs = swapped(after(mine, pieces[1]))
    turn = (jnp.arange(nz) == lax.axis_index("z")).astype(f32)[:, None, None]
    gain_rows = (turn * in_three(gain_part)).reshape(3 * nz, feats).astype(bf16)
    d_pre, g = run(
        grad_up_kernel, [(toks, hid), (ntp, hid + 3 * nz, feats)],
        place, mine, theirs, wd, hidden_pre, gain_rows,
    )
    g = lax.psum_scatter(g.reshape(-1, feats), "z", scatter_dimension=0, tiled=True)

    pieces[1], left = after(pieces[1], d_pre), after(wu, d_pre)
    for d in range(1, ny // 2):
        pieces[d + 1] = shifted(pieces[d], "y", 1)
        pieces[ny - d] = left = shifted(left, "y", -1)
    mine = gather_directly(d_pre, "x")
    theirs = swapped(after(mine, pieces))
    [grad_input] = run(
        grad_input_kernel, [(toks, feats)], place, mine, theirs, *pieces,
        scratch=[(nz, hid, feats)],
    )

    rows = hid // ny
    gain = summed(g[hid:].reshape(nz, 3, feats))
    gain = in_three(jnp.sum(gain, axis=0)).astype(bf16)
    gain = jnp.broadcast_to(jnp.pad(gain, ((0, 5), (0, 0))), (ny, 8, feats))
    g = jnp.concatenate([g[:hid].reshape(ny, rows, feats), gain], axis=1)
    g = summed(exchange(g, "y")) * scaled
    grad_gain = jnp.sum(g[rows : rows + 3], axis=0)
    grad_up = lax.ppermute(g[:rows], ("z", "x", "c"), swap).T
    return (grad_input, grad_up, grad_gain)


def solution(mesh):
    torus = Mesh(mesh.devices.reshape(8, 8, mesh.shape["tp"] // 2, 2), ("z", "y", "x", "c"))
    in_specs = (
        P(FS, TP),
        P(FS, TP),
        P(FS, TP),
        P(TP),
        P(TP, FS),
        P(TP, FS),
        P(FS, TP),
    )
    out_specs = (P(FS, TP), P(TP, FS), P(TP))
    return jax.shard_map(
        one_device, mesh=torus, in_specs=in_specs, out_specs=out_specs, check_vma=False
    )
```
